32 devices in a mesh: grp: 1, ep: 4 (over z), tp: 8 (over y, x, core).
Axes of the slice: x: 2, y: 2, z: 4, core: 2. Of those that a mesh axis runs over, the one named last changes fastest.
Arguments:
- tokens: bfloat16 [256, 2048], P(('grp', 'ep')), may hold values from -6 to 6
- norm_gain: float32 [2048], replicated, may hold values from 0.1 to 1.9
- routes: int32 [256, 8], P(('grp', 'ep')), may hold values from 0 to 15, all different within a row; in each aligned block of 64 rows (0 to 63, 64 to 127, ...) at most 64 rows name the same one
- route_weight: float32 [256, 8], P(('grp', 'ep')), may hold values from 0.05 to 1
- gate_proj: bfloat16 [32, 2048, 256], P(('ep', 'tp')), may hold values from -0.125 to 0.125
- up_proj: bfloat16 [32, 2048, 256], P(('ep', 'tp')), may hold values from -0.125 to 0.125
- down_proj: bfloat16 [32, 256, 2048], P(('ep', 'tp')), may hold values from -0.25 to 0.25
- shared_gate: bfloat16 [2048, 512], P(None, 'tp'), may hold values from -0.125 to 0.125
- shared_up: bfloat16 [2048, 512], P(None, 'tp'), may hold values from -0.125 to 0.125
- shared_down: bfloat16 [512, 2048], P('tp'), may hold values from -0.25 to 0.25
Outputs:
- mixed: bfloat16 [256, 2048], P(('grp', 'ep'), 'tp')
The draws below stay inside these ranges and needn't reach their ends.
Inputs may be any that keep to these rules, and one draw needn't show every extreme that they name: `routes`: each row names 8 different experts. Among the 64 rows of one ep index no expert is named by more than 64 rows, a bound that some block reaches of them.
All inputs are finite; a program needn't handle non-finite values.
Results may differ from the reference program's by a relative error of at most 0.0064.
Values may be sent and summed in bfloat16 or wider, within the bound.
A program may use at most 64 MiB of HBM per device.

```python
import math
import jax
import jax.numpy as jnp
import numpy as np
from jax import lax

D = 2048
FF = 512
SHARED = 512
TOP_K = 8
EXPERT_SHARDS = 2
TOK_DEV = 64
TOKENS = 256
EXPERTS = 16
CAP = 64
N_EP = 4


def block_levels(key, dims, cuts, least, top_value):
    def one(dim, shards_of):
        draws = jax.random.uniform(jax.random.fold_in(jax.random.fold_in(key, 6), dim), (shards_of,), jnp.float32, least / len(cuts), top_value / len(cuts))
        return jnp.repeat(jnp.exp(draws), dims[dim] // shards_of).reshape((-1,) + (1,) * (len(dims) - dim - 1))

    factor_of = one(*cuts[0])
    for cut in cuts[1:]:
        factor_of = factor_of * one(*cut)
    return factor_of


def routed_block(rng, own, number, rows, number_of, top, limit, skew):
    order = jax.random.permutation(rng, number_of)
    heavy_load, ordinary = portions_of(number_of, rows * top, limit, skew, True), portions_of(number_of, rows * top, limit, skew, False)
    places = jnp.arange(number_of)

    def named(lengths, turn):
        used = int((lengths > 0).sum())
        fixed = max(1, used // 4)
        passed = fixed + (places - fixed + turn * (used - fixed)) % max(1, number_of - fixed)
        return jnp.zeros((number_of,), jnp.int32).at[order[jnp.where(places < fixed, places, passed)]].set(jnp.asarray(lengths, jnp.int32))

    lengths = jnp.where(number % 4 == 0, named(heavy_load, number // 4), named(ordinary, number - number // 4 - 1))
    mixed = jax.random.permutation(jax.random.fold_in(own, 3), number_of)
    giver, sink = mixed[0:number_of // 2 * 2:2], mixed[1:number_of // 2 * 2:2]
    margin = jnp.minimum(lengths[giver] - 1, limit - lengths[sink]) // 2
    margin = jnp.where((giver == order[0]) | (sink == order[0]) | (lengths[sink] == 0), 0, jnp.maximum(margin, 0))
    passed = jax.random.randint(jax.random.fold_in(own, 4), (number_of // 2,), 0, 1 << 20) % (margin + 1)
    lengths = lengths.at[giver].add(-passed).at[sink].add(passed)
    labels = jnp.searchsorted(jnp.cumsum(lengths), jnp.arange(rows * top), side="right").astype(jnp.int32)
    grid = labels.reshape(top, rows).T
    grid = grid[jax.random.permutation(jax.random.fold_in(own, 1), rows)]
    turn = jax.random.randint(jax.random.fold_in(own, 2), (rows, 1), 0, top)
    return jnp.take_along_axis(grid, (jnp.arange(top)[None, :] + turn) % top, axis=1)


def portions_of(count, total, bound, lean, full):
    weights = [(1 << 20) // math.isqrt(standing ** lean) + 1 for standing in range(1, count + 1)]
    largest = bound if full else min(bound, max(-(-total // count), total * weights[0] // sum(weights)))
    least = 1 if total - largest >= count - 1 else 0
    holding, surplus = [largest] + [least] * (count - 1), total - largest - least * (count - 1)
    while surplus > 0:
        free = [i for i in range(1, count) if holding[i] < largest] or [i for i in range(1, count) if holding[i] < bound]
        whole, remaining = sum([weights[i] for i in free]), surplus
        for i in free:
            more = min(bound - holding[i], max(1, remaining * weights[i] // whole), surplus)
            holding[i] = holding[i] + more
            surplus = surplus - more
    return np.array(holding)


def gaussian(own_key, dims, scale, most, pieces=(), dtype=jnp.bfloat16):
    level = block_levels(own_key, dims, pieces, -0.22, 0.18) if pieces else 1.0
    values = jax.random.normal(own_key, dims, jnp.float32) * scale * level
    return jnp.minimum(jnp.maximum(values, -most), most).astype(dtype)


def setup_inputs(seed: int = 0, part: int = 0) -> dict:
    streams_of = jax.random.split(jax.random.key(seed), 11)
    own_keys = jax.random.split(jax.random.fold_in(streams_of[10], part), 11)
    tokens = gaussian(own_keys[0], (TOKENS, D), 1.0, 6.0, ((0, 4),))
    norm_gain = jnp.clip(1.0 + 0.18 * jax.random.normal(streams_of[1], (D,), jnp.float32), 0.1, 1.9)
    routes_keys = jax.random.split(jax.random.fold_in(own_keys[2], 1), TOKENS // TOK_DEV)
    routes_turns = jax.random.permutation(jax.random.fold_in(own_keys[2], 3), TOKENS // TOK_DEV)
    routes = jax.vmap(lambda own, number: routed_block(jax.random.fold_in(own_keys[2], 2), own, number, TOK_DEV, EXPERTS, TOP_K, CAP, 2))(routes_keys, routes_turns).reshape((TOKENS, TOP_K))
    route_weight = jnp.clip(jnp.exp(math.log(1.0) - 2.9957323 * jax.random.uniform(own_keys[3], (TOKENS, TOP_K), jnp.float32) ** block_levels(own_keys[3], (TOKENS, TOP_K), ((0, 4),), -0.2, 0.2)), 0.05, 1.0)
    gate_proj = gaussian(streams_of[4], (EXPERTS * EXPERT_SHARDS, D, FF // EXPERT_SHARDS), D ** -0.5, 0.125, ((0, 32),))
    up_proj = gaussian(streams_of[5], (EXPERTS * EXPERT_SHARDS, D, FF // EXPERT_SHARDS), D ** -0.5, 0.125, ((0, 32),))
    down_proj = gaussian(streams_of[6], (EXPERTS * EXPERT_SHARDS, FF // EXPERT_SHARDS, D), FF ** -0.5, 0.25, ((0, 32),))
    shared_gate = gaussian(streams_of[7], (D, SHARED), D ** -0.5, 0.125, ((1, 8),))
    shared_up = gaussian(streams_of[8], (D, SHARED), D ** -0.5, 0.125, ((1, 8),))
    shared_down = gaussian(streams_of[9], (SHARED, D), SHARED ** -0.5, 0.25, ((0, 8),))
    return {"tokens": tokens, "norm_gain": norm_gain, "routes": routes, "route_weight": route_weight, "gate_proj": gate_proj, "up_proj": up_proj, "down_proj": down_proj, "shared_gate": shared_gate, "shared_up": shared_up, "shared_down": shared_down}


eps = 1e-06
routed_scale = 2.5

def expert_apply(row_block, gate_half, up_half, down_half):
    gate_part = jnp.dot(row_block, gate_half, preferred_element_type=jnp.float32)
    upper = jnp.dot(row_block, up_half, preferred_element_type=jnp.float32)
    active = (jax.nn.silu(gate_part) * upper).astype(jnp.bfloat16)
    return jnp.dot(active, down_half, preferred_element_type=jnp.float32)

def reference(tokens, norm_gain, routes, route_weight, gate_proj, up_proj, down_proj, shared_gate, shared_up, shared_down):
    values = tokens.astype(jnp.float32)
    scaled = values * lax.rsqrt(lax.optimization_barrier(jnp.mean(values * values, axis=-1, keepdims=True)) + eps)
    normed = (scaled * norm_gain).astype(jnp.bfloat16)
    mixing = route_weight / lax.optimization_barrier(jnp.sum(route_weight, axis=1, keepdims=True)) * routed_scale
    row_limit = N_EP * CAP

    def one_expert(expert_id, total):
        expert_id = jnp.asarray(expert_id).astype(jnp.int32)
        hit_table = routes == expert_id
        taken_rows = jnp.any(hit_table, axis=1)
        token_weight = lax.optimization_barrier(jnp.sum(jnp.where(hit_table, mixing, 0.0), axis=1))
        picked = jnp.nonzero(taken_rows, size=row_limit, fill_value=0)[0].astype(jnp.int32)
        live_rows = jnp.arange(row_limit) < jnp.sum(taken_rows.astype(jnp.int32))
        row_block = normed[picked]
        produced = jnp.zeros((row_limit, D), jnp.float32)
        for half_index in range(EXPERT_SHARDS):
            weight_row = (expert_id * EXPERT_SHARDS + half_index).astype(jnp.int32)
            gate_half = lax.dynamic_index_in_dim(gate_proj, weight_row, 0, keepdims=False)
            up_half = lax.dynamic_index_in_dim(up_proj, weight_row, 0, keepdims=False)
            down_half = lax.dynamic_index_in_dim(down_proj, weight_row, 0, keepdims=False)
            produced = produced + expert_apply(row_block, gate_half, up_half, down_half)
        scale_rows = jnp.where(live_rows, token_weight[picked], 0.0)
        return total.at[picked].add(produced * scale_rows[:, None])
    routed = lax.fori_loop(0, EXPERTS, one_expert, jnp.zeros((TOKENS, D), jnp.float32))
    shared_term = expert_apply(normed, shared_gate, shared_up, shared_down)
    return (routed + shared_term).astype(jnp.bfloat16)
```

```python
import functools

import jax
import jax.numpy as jnp
from jax import lax
from jax.experimental import pallas as pl
from jax.experimental.pallas import tpu as pltpu
from jax.sharding import PartitionSpec as P

EXPERT_SHARDS = 2
CORES = 2
MESH = pl.DeviceIdType.MESH

eps = 1e-06
routed_scale = 2.5


def norm_rows(tokens, norm_gain):
    values = tokens.astype(jnp.float32)
    scaled = values * lax.rsqrt(jnp.mean(values * values, axis=-1, keepdims=True) + eps)
    return (scaled * norm_gain).astype(jnp.bfloat16)


def silu(value):
    return value / (1.0 + jnp.exp(-value))


def kernel(
    n_ep,
    n_tp,
    tok_hbm,
    gain_hbm,
    routes_hbm,
    score_hbm,
    gate_hbm,
    up_hbm,
    down_hbm,
    sgate_hbm,
    sup_hbm,
    sdown_hbm,
    out_ref,
    tok,
    gain,
    routes,
    score,
    gate,
    up,
    down,
    sgate,
    sup,
    sdown,
    gathered,
    part,
    part_in,
    pair,
    pair_in,
    plane,
    plane_in,
    kept,
    load_sem,
    z_send,
    z_recv,
    xy_send,
    xy_recv,
    d2d_send,
    d2d_recv,
    a_send,
    a_recv,
    b_send,
    b_recv,
    c_send,
    c_recv,
):
    chips = n_tp // CORES
    me = lax.axis_index("ep")
    seat = lax.axis_index("tp")
    chip, core = seat // CORES, seat % CORES
    rows, width = tok.shape
    half = rows // CORES
    chip_cols = width // chips
    out_cols = width // n_tp
    groups = group_count(n_ep)
    span = (n_ep - 1) // groups
    expert = me * (n_tp // EXPERT_SHARDS) + chip

    partner = {"tp": chip * CORES + 1 - core}
    plane_chip = [lax.rem(chip + j, chips) for j in range(chips)]
    plane_peer = [{"tp": c * CORES + core} for c in plane_chip]
    forward = [{"ep": lax.rem(me + d, n_ep)} for d in range(n_ep)]
    backward = [{"ep": lax.rem(me + n_ep - d, n_ep)} for d in range(n_ep)]

    def remote(src, dst, send, recv, target):
        return pltpu.make_async_remote_copy(
            src_ref=src, dst_ref=dst, send_sem=send, recv_sem=recv, device_id=target, device_id_type=MESH
        )

    loads = [
        pltpu.make_async_copy(src, dst, load_sem.at[i])
        for i, (src, dst) in enumerate(
            [
                (tok_hbm, tok),
                (routes_hbm, routes.at[0]),
                (score_hbm, score.at[0]),
                (gain_hbm, gain),
                (gate_hbm.at[0], gate),
                (up_hbm.at[0], up),
                (sgate_hbm, sgate),
                (sup_hbm, sup),
                (down_hbm.at[0], down),
                (sdown_hbm, sdown),
            ]
        )
    ]
    for load in loads:
        load.start()

    barrier = pltpu.get_barrier_semaphore()
    targets = forward[1:] + plane_peer[1:] + [partner]
    for target in targets:
        pl.semaphore_signal(barrier, inc=1, device_id=target, device_id_type=MESH)
    for load in loads[:3]:
        load.wait()
    pl.semaphore_wait(barrier, len(targets))

    my_rows = pl.ds(pl.multiple_of(core * half, half), half)
    my_cols = pl.ds(pl.multiple_of(chip * chip_cols, chip_cols), chip_cols)

    z_copies = []
    for d in range(1, n_ep):
        z_copies.append(
            [
                remote(
                    tok.at[my_rows, my_cols],
                    gathered.at[d - 1, my_rows, my_cols],
                    z_send.at[0, d - 1],
                    z_recv.at[0, d - 1],
                    forward[d],
                ),
                remote(routes.at[0], routes.at[d], z_send.at[1, d - 1], z_recv.at[1, d - 1], forward[d]),
                remote(score.at[0], score.at[d], z_send.at[2, d - 1], z_recv.at[2, d - 1], forward[d]),
            ]
        )
    for copies in z_copies:
        for copy in copies:
            copy.start()

    diagonal = lax.broadcasted_iota(jnp.int32, (rows, rows), 0) == lax.broadcasted_iota(
        jnp.int32, (rows, rows), 1
    )

    def row_weight(slot):
        scores = score[slot]
        mixing = scores / jnp.sum(scores, axis=0, keepdims=True) * routed_scale
        lane = jnp.sum(jnp.where(routes[slot] == expert, mixing, 0.0), axis=0, keepdims=True)
        return jnp.sum(jnp.where(diagonal, lane, 0.0), axis=1, keepdims=True)

    def span_of(group):
        if group == 0:
            return 0, 1
        return 1 + (group - 1) * span, span

    a_copies, b_copies = [], []

    def compute(group):
        first, count = span_of(group)
        raw = tok[...] if group == 0 else gathered[first - 1 : first - 1 + count].reshape(count * rows, width)
        normed = norm_rows(raw, gain[...])
        if group == 0:
            for load in loads[4:8]:
                load.wait()
        gate_part = jnp.dot(normed, gate[...], preferred_element_type=jnp.float32)
        upper = jnp.dot(normed, up[...], preferred_element_type=jnp.float32)
        weight = [row_weight(slot) for slot in range(first, first + count)]
        weight = weight[0] if count == 1 else jnp.concatenate(weight, axis=0)
        active = (silu(gate_part) * upper * weight).astype(jnp.bfloat16)
        if group == 0:
            contract = (((1,), (1,)), ((), ()))
            shared_gate = lax.dot_general(normed, sgate[...], contract, preferred_element_type=jnp.float32)
            shared_up = lax.dot_general(normed, sup[...], contract, preferred_element_type=jnp.float32)
            shared = (silu(shared_gate) * shared_up).astype(jnp.bfloat16)
            for load in loads[8:]:
                load.wait()
        for c in range(chips):
            cols = slice(c * chip_cols, (c + 1) * chip_cols)
            value = jnp.dot(active, down[:, cols], preferred_element_type=jnp.float32)
            if group == 0:
                value = value + jnp.dot(shared, sdown[:, cols], preferred_element_type=jnp.float32)
            value = value.astype(jnp.bfloat16)
            for s in range(count):
                for k in range(CORES):
                    part[first + s, k, c] = value[
                        s * rows : (s + 1) * rows, k * out_cols : (k + 1) * out_cols
                    ]
        copy = remote(
            part.at[pl.ds(first, count), 1 - core],
            part_in.at[pl.ds(first, count)],
            a_send.at[group],
            a_recv.at[group],
            partner,
        )
        copy.start()
        a_copies.append(copy)

    def pair_sum(slots, c):
        return part[slots, core, c].astype(jnp.float32) + part_in[slots, c].astype(jnp.float32)

    def reduce_pair(group):
        first, count = span_of(group)
        slots = pl.ds(first, count)
        a_copies[group].wait_recv()
        copies = []
        for j in range(1, chips):
            c = plane_chip[j]
            pair[slots, c] = pair_sum(slots, c).astype(jnp.bfloat16)
            copy = remote(
                pair.at[slots, c],
                pair_in.at[slots, j - 1],
                b_send.at[group, j - 1],
                b_recv.at[group, j - 1],
                plane_peer[j],
            )
            copy.start()
            copies.append(copy)
        b_copies.append(copies)

    c_copies = []

    def reduce_plane(group):
        first, count = span_of(group)
        slots = pl.ds(first, count)
        total = pair_sum(slots, chip)
        for j in range(1, chips):
            b_copies[group][j - 1].wait_recv()
            total = total + pair_in[slots, j - 1].astype(jnp.float32)
        if group == 0:
            kept[...] = total[0]
            return
        plane[pl.ds(first - 1, count)] = total.astype(jnp.bfloat16)
        for d in range(first, first + count):
            copy = remote(
                plane.at[d - 1], plane_in.at[d - 1], c_send.at[d - 1], c_recv.at[d - 1], backward[d]
            )
            copy.start()
            c_copies.append(copy)

    xy_copies = []

    def spread(group):
        first, count = span_of(group)
        for d in range(first, first + count):
            z_copies[d - 1][0].wait_recv()
        block = gathered.at[pl.ds(first - 1, count), my_rows, my_cols]
        copies = []
        for j in range(1, chips):
            copy = remote(
                block, block, xy_send.at[group - 1, j - 1], xy_recv.at[group - 1, j - 1], plane_peer[j]
            )
            copy.start()
            copies.append(copy)
        xy_copies.append(copies)

    d2d_copies = []

    def swap(group):
        first, count = span_of(group)
        for copy in xy_copies[group - 1]:
            copy.wait_recv()
        block = gathered.at[pl.ds(first - 1, count), my_rows]
        copy = remote(block, block, d2d_send.at[group - 1], d2d_recv.at[group - 1], partner)
        copy.start()
        d2d_copies.append(copy)

    def arrive(group):
        first, count = span_of(group)
        for d in range(first, first + count):
            z_copies[d - 1][1].wait_recv()
            z_copies[d - 1][2].wait_recv()
        d2d_copies[group - 1].wait_recv()

    loads[3].wait()
    compute(0)
    for group in range(1, groups + 1):
        spread(group)
    reduce_pair(0)
    swap(1)
    for group in range(1, groups + 1):
        if group < groups:
            swap(group + 1)
        if group > 1:
            reduce_pair(group - 1)
        arrive(group)
        compute(group)
        if group > 1:
            reduce_plane(group - 1)
    reduce_pair(groups)
    reduce_plane(0)
    reduce_plane(groups)
    total = kept[...]
    for d in range(1, n_ep):
        c_copies[d - 1].wait_recv()
        total = total + plane_in[d - 1].astype(jnp.float32)
    out_ref[...] = total.astype(jnp.bfloat16)
    everything = sum(z_copies + xy_copies + b_copies, []) + d2d_copies + a_copies + c_copies
    for copy in everything:
        copy.wait_send()


def group_count(n_ep):
    return 3 if (n_ep - 1) % 3 == 0 else n_ep - 1


def per_device(
    tokens,
    norm_gain,
    routes,
    route_weight,
    gate_proj,
    up_proj,
    down_proj,
    shared_gate,
    shared_up,
    shared_down,
):
    n_ep = lax.axis_size("ep")
    n_tp = lax.axis_size("tp")
    chips = n_tp // CORES
    rows, width = tokens.shape
    out_cols = width // n_tp
    top_count = routes.shape[1]
    hidden = gate_proj.shape[2]
    shared = shared_gate.shape[1]
    groups = group_count(n_ep)
    bf16, f32 = jnp.bfloat16, jnp.float32
    dma = pltpu.SemaphoreType.DMA
    operands = (
        tokens,
        norm_gain.reshape(1, width),
        routes.T,
        route_weight.T,
        gate_proj,
        up_proj,
        down_proj,
        shared_gate.T,
        shared_up.T,
        shared_down,
    )
    return pl.pallas_call(
        functools.partial(kernel, n_ep, n_tp),
        out_shape=jax.ShapeDtypeStruct((rows, out_cols), bf16),
        in_specs=[pl.BlockSpec(memory_space=pl.ANY)] * len(operands),
        out_specs=pl.BlockSpec(memory_space=pltpu.VMEM),
        scratch_shapes=[
            pltpu.VMEM((rows, width), bf16),
            pltpu.VMEM((1, width), f32),
            pltpu.VMEM((n_ep, top_count, rows), jnp.int32),
            pltpu.VMEM((n_ep, top_count, rows), f32),
            pltpu.VMEM((width, hidden), bf16),
            pltpu.VMEM((width, hidden), bf16),
            pltpu.VMEM((hidden, width), bf16),
            pltpu.VMEM((shared, width), bf16),
            pltpu.VMEM((shared, width), bf16),
            pltpu.VMEM((shared, width), bf16),
            pltpu.VMEM((n_ep - 1, rows, width), bf16),
            pltpu.VMEM((n_ep, CORES, chips, rows, out_cols), bf16),
            pltpu.VMEM((n_ep, chips, rows, out_cols), bf16),
            pltpu.VMEM((n_ep, chips, rows, out_cols), bf16),
            pltpu.VMEM((n_ep, chips - 1, rows, out_cols), bf16),
            pltpu.VMEM((n_ep - 1, rows, out_cols), bf16),
            pltpu.VMEM((n_ep - 1, rows, out_cols), bf16),
            pltpu.VMEM((rows, out_cols), f32),
            dma((len(operands),)),
            dma((3, n_ep - 1)),
            dma((3, n_ep - 1)),
            dma((groups, chips - 1)),
            dma((groups, chips - 1)),
            dma((groups,)),
            dma((groups,)),
            dma((groups + 1,)),
            dma((groups + 1,)),
            dma((groups + 1, chips - 1)),
            dma((groups + 1, chips - 1)),
            dma((n_ep - 1,)),
            dma((n_ep - 1,)),
        ],
        compiler_params=pltpu.CompilerParams(
            collective_id=0, has_side_effects=True, vmem_limit_bytes=60 * 1024 * 1024
        ),
    )(*operands)


def solution(mesh):
    in_specs = (
        P(("grp", "ep"), None),
        P(),
        P(("grp", "ep"), None),
        P(("grp", "ep"), None),
        P(("ep", "tp"), None, None),
        P(("ep", "tp"), None, None),
        P(("ep", "tp"), None, None),
        P(None, "tp"),
        P(None, "tp"),
        P("tp", None),
    )
    out_specs = P(("grp", "ep"), "tp")
    return jax.shard_map(
        per_device, mesh=mesh, in_specs=in_specs, out_specs=out_specs, check_vma=False
    )
```

```python
import functools

import jax
import jax.numpy as jnp
from jax import lax
from jax.experimental import pallas as pl
from jax.experimental.pallas import tpu as pltpu
from jax.sharding import PartitionSpec as P

EXPERT_SHARDS = 2
CORES = 2
MESH = pl.DeviceIdType.MESH

eps = 1e-06
routed_scale = 2.5


def norm_rows(tokens, norm_gain):
    values = tokens.astype(jnp.float32)
    scaled = values * lax.rsqrt(jnp.mean(values * values, axis=-1, keepdims=True) + eps)
    return (scaled * norm_gain).astype(jnp.bfloat16)


def silu(value):
    return value / (1.0 + jnp.exp(-value))


def kernel(
    n_ep,
    n_tp,
    tok_hbm,
    gain_hbm,
    routes_hbm,
    score_hbm,
    gate_hbm,
    up_hbm,
    down_hbm,
    sgate_hbm,
    sup_hbm,
    sdown_hbm,
    out_ref,
    tok,
    gain,
    routes,
    score,
    gate,
    up,
    down,
    sgate,
    sup,
    sdown,
    gathered,
    part,
    part_in,
    pair,
    pair_in,
    plane,
    plane_in,
    kept,
    load_sem,
    z_send,
    z_recv,
    xy_send,
    xy_recv,
    d2d_send,
    d2d_recv,
    a_send,
    a_recv,
    b_send,
    b_recv,
    c_send,
    c_recv,
):
    chips = n_tp // CORES
    me = lax.axis_index("ep")
    seat = lax.axis_index("tp")
    chip, core = seat // CORES, seat % CORES
    rows, width = tok.shape
    half = rows // CORES
    chip_cols = width // chips
    out_cols = width // n_tp
    groups = group_count(n_ep)
    span = (n_ep - 1) // groups
    expert = me * (n_tp // EXPERT_SHARDS) + chip

    partner = {"tp": chip * CORES + 1 - core}
    plane_chip = [flipped(chip, j, chips) for j in range(chips)]
    plane_order = list(range(chips - 1, 0, -1))
    plane_peer = [{"tp": c * CORES + core} for c in plane_chip]
    others = [lax.rem(me + d, n_ep) for d in range(n_ep)]
    forward = [{"ep": other} for other in others]

    def remote(src, dst, send, recv, target):
        return pltpu.make_async_remote_copy(
            src_ref=src, dst_ref=dst, send_sem=send, recv_sem=recv, device_id=target, device_id_type=MESH
        )

    loads = [
        pltpu.make_async_copy(src, dst, load_sem.at[i])
        for i, (src, dst) in enumerate(
            [
                (tok_hbm, tok),
                (routes_hbm, routes.at[0]),
                (score_hbm, score.at[0]),
                (gain_hbm, gain),
                (gate_hbm.at[0], gate),
                (up_hbm.at[0], up),
                (sgate_hbm, sgate),
                (sup_hbm, sup),
                (down_hbm.at[0], down),
                (sdown_hbm, sdown),
            ]
        )
    ]
    for load in loads:
        load.start()

    barrier = pltpu.get_barrier_semaphore()
    targets = forward[1:] + plane_peer[1:] + [partner]
    for target in targets:
        pl.semaphore_signal(barrier, inc=1, device_id=target, device_id_type=MESH)
    for load in loads[:3]:
        load.wait()
    pl.semaphore_wait(barrier, len(targets))

    my_rows = pl.ds(pl.multiple_of(core * half, half), half)
    my_cols = pl.ds(pl.multiple_of(chip * chip_cols, chip_cols), chip_cols)

    def z_pieces(source, slot, target):
        return [
            remote(
                tok.at[my_rows, my_cols],
                gathered.at[slot - 1, my_rows, my_cols],
                z_send.at[0, source],
                z_recv.at[0, slot - 1],
                target,
            ),
            remote(routes.at[0], routes.at[slot], z_send.at[1, source], z_recv.at[1, slot - 1], target),
            remote(score.at[0], score.at[slot], z_send.at[2, source], z_recv.at[2, slot - 1], target),
        ]

    z_copies = [z_pieces(d - 1, place_of(me, others[d], n_ep), forward[d]) for d in range(1, n_ep)]
    z_arrivals = [z_pieces(slot - 1, slot, forward[1]) for slot in range(1, n_ep)]
    for piece in range(3):
        for copies in z_copies:
            copies[piece].start()

    diagonal = lax.broadcasted_iota(jnp.int32, (rows, rows), 0) == lax.broadcasted_iota(
        jnp.int32, (rows, rows), 1
    )

    def row_weight(slot):
        scores = score[slot]
        mixing = scores / jnp.sum(scores, axis=0, keepdims=True) * routed_scale
        lane = jnp.sum(jnp.where(routes[slot] == expert, mixing, 0.0), axis=0, keepdims=True)
        return jnp.sum(jnp.where(diagonal, lane, 0.0), axis=1, keepdims=True)

    def span_of(group):
        if group == 0:
            return 0, 1
        return 1 + (group - 1) * span, span

    a_copies, b_copies = [], []

    def compute(group):
        first, count = span_of(group)
        raw = tok[...] if group == 0 else gathered[first - 1 : first - 1 + count].reshape(count * rows, width)
        normed = norm_rows(raw, gain[...])
        if group == 0:
            for load in loads[4:8]:
                load.wait()
        gate_part = jnp.dot(normed, gate[...], preferred_element_type=jnp.float32)
        upper = jnp.dot(normed, up[...], preferred_element_type=jnp.float32)
        weight = [row_weight(slot) for slot in range(first, first + count)]
        weight = weight[0] if count == 1 else jnp.concatenate(weight, axis=0)
        active = (silu(gate_part) * upper * weight).astype(jnp.bfloat16)
        if group == 0:
            contract = (((1,), (1,)), ((), ()))
            shared_gate = lax.dot_general(normed, sgate[...], contract, preferred_element_type=jnp.float32)
            shared_up = lax.dot_general(normed, sup[...], contract, preferred_element_type=jnp.float32)
            shared = (silu(shared_gate) * shared_up).astype(jnp.bfloat16)
            for load in loads[8:]:
                load.wait()
        copies = [None] * chips
        for j in plane_order + [0]:
            c = plane_chip[j]
            cols = pl.ds(pl.multiple_of(c * chip_cols, chip_cols), chip_cols)
            value = jnp.dot(active, down[:, cols], preferred_element_type=jnp.float32)
            if group == 0:
                value = value + jnp.dot(shared, sdown[:, cols], preferred_element_type=jnp.float32)
            value = value.astype(jnp.bfloat16)
            for s in range(count):
                for k in range(CORES):
                    part[first + s, k, c] = value[
                        s * rows : (s + 1) * rows, k * out_cols : (k + 1) * out_cols
                    ]
            copies[j] = remote(
                part.at[pl.ds(first, count), 1 - core, c],
                part_in.at[pl.ds(first, count), c],
                a_send.at[group, j],
                a_recv.at[group, j],
                partner,
            )
            copies[j].start()
        a_copies.append(copies)

    def pair_sum(slots, c):
        return part[slots, core, c].astype(jnp.float32) + part_in[slots, c].astype(jnp.float32)

    def reduce_pair(group):
        first, count = span_of(group)
        slots = pl.ds(first, count)
        copies = [None] * chips
        for j in plane_order:
            c = plane_chip[j]
            a_copies[group][j].wait_recv()
            pair[slots, c] = pair_sum(slots, c).astype(jnp.bfloat16)
            copies[j] = remote(
                pair.at[slots, c],
                pair_in.at[slots, j - 1],
                b_send.at[group, j - 1],
                b_recv.at[group, j - 1],
                plane_peer[j],
            )
            copies[j].start()
        a_copies[group][0].wait_recv()
        b_copies.append(copies)

    c_copies = []

    def reduce_plane(group):
        first, count = span_of(group)
        slots = pl.ds(first, count)
        total = pair_sum(slots, chip)
        for j in range(1, chips):
            b_copies[group][j].wait_recv()
            total = total + pair_in[slots, j - 1].astype(jnp.float32)
        if group == 0:
            kept[...] = total[0]
            return
        plane[pl.ds(first - 1, count)] = total.astype(jnp.bfloat16)
        for d in range(first, first + count):
            source = source_of(me, d, n_ep)
            there = lax.rem(source - me + n_ep, n_ep) - 1
            copy = remote(
                plane.at[d - 1], plane_in.at[there], c_send.at[d - 1], c_recv.at[there], {"ep": source}
            )
            copy.start()
            c_copies.append(copy)

    xy_copies, d2d_copies = [], []

    def block_of(group, c):
        first, count = span_of(group)
        cols = pl.ds(pl.multiple_of(c * chip_cols, chip_cols), chip_cols)
        return gathered.at[pl.ds(first - 1, count), my_rows, cols]

    def swap_piece(group, j):
        block = block_of(group, plane_chip[j])
        copy = remote(block, block, d2d_send.at[group - 1, j], d2d_recv.at[group - 1, j], partner)
        copy.start()
        d2d_copies[group - 1].append(copy)

    def spread(group):
        first, count = span_of(group)
        for d in range(first, first + count):
            z_arrivals[d - 1][0].wait_recv()
        block = block_of(group, chip)
        copies = [None] * chips
        for j in plane_order:
            copies[j] = remote(
                block, block, xy_send.at[group - 1, j - 1], xy_recv.at[group - 1, j - 1], plane_peer[j]
            )
            copies[j].start()
        xy_copies.append(copies)
        d2d_copies.append([])
        swap_piece(group, 0)

    def swap(group):
        for j in plane_order[::-1]:
            xy_copies[group - 1][j].wait_recv()
            swap_piece(group, j)

    def arrive(group):
        first, count = span_of(group)
        for d in range(first, first + count):
            z_arrivals[d - 1][1].wait_recv()
            z_arrivals[d - 1][2].wait_recv()
        for copy in d2d_copies[group - 1]:
            copy.wait_recv()

    loads[3].wait()
    compute(0)
    for group in range(1, groups + 1):
        spread(group)
    reduce_pair(0)
    swap(1)
    for group in range(1, groups + 1):
        if group < groups:
            swap(group + 1)
        if group > 1:
            reduce_pair(group - 1)
        arrive(group)
        compute(group)
    reduce_plane(0)
    for group in range(1, groups):
        if group == groups - 1:
            reduce_pair(groups)
        reduce_plane(group)
    reduce_plane(groups)
    total = kept[...]
    for d in range(1, n_ep):
        remote(
            plane.at[0], plane_in.at[d - 1], c_send.at[d - 1], c_recv.at[d - 1], forward[1]
        ).wait_recv()
        total = total + plane_in[d - 1].astype(jnp.float32)
    out_ref[...] = total.astype(jnp.bfloat16)
    everything = sum(z_copies + xy_copies + b_copies + d2d_copies + a_copies, []) + c_copies
    for copy in everything:
        if copy is not None:
            copy.wait_send()


def flipped(chip, j, chips):
    assert chips & (chips - 1) == 0
    out, bit = chip, 1
    while bit < chips:
        if j & bit:
            out = out + bit - 2 * bit * (chip // bit % 2)
        bit *= 2
    return out


def room(index, count):
    side = jnp.minimum(index, count - 1 - index)
    toward = jnp.where(index < count - 1 - index, 1, -1)
    return side, toward


def source_of(index, place, count):
    side, toward = room(index, count)
    near = (place + 1) // 2 * (1 if place % 2 else -1)
    return index + toward * jnp.where(place <= 2 * side, near, place - side)


def place_of(source, index, count):
    side, toward = room(index, count)
    away = jnp.abs(source - index)
    same = (source - index) * toward > 0
    return jnp.where(away <= side, 2 * away - jnp.where(same, 1, 0), away + side)


def group_count(n_ep):
    return 3 if (n_ep - 1) % 3 == 0 else n_ep - 1


def per_device(
    tokens,
    norm_gain,
    routes,
    route_weight,
    gate_proj,
    up_proj,
    down_proj,
    shared_gate,
    shared_up,
    shared_down,
):
    n_ep = lax.axis_size("ep")
    n_tp = lax.axis_size("tp")
    chips = n_tp // CORES
    rows, width = tokens.shape
    out_cols = width // n_tp
    top_count = routes.shape[1]
    hidden = gate_proj.shape[2]
    shared = shared_gate.shape[1]
    groups = group_count(n_ep)
    bf16, f32 = jnp.bfloat16, jnp.float32
    dma = pltpu.SemaphoreType.DMA
    operands = (
        tokens,
        norm_gain.reshape(1, width),
        routes.T,
        route_weight.T,
        gate_proj,
        up_proj,
        down_proj,
        shared_gate.T,
        shared_up.T,
        shared_down,
    )
    return pl.pallas_call(
        functools.partial(kernel, n_ep, n_tp),
        out_shape=pltpu.VMEM((rows, out_cols), bf16),
        in_specs=[pl.BlockSpec(memory_space=pl.ANY)] * len(operands),
        out_specs=pl.BlockSpec(memory_space=pltpu.VMEM),
        scratch_shapes=[
            pltpu.VMEM((rows, width), bf16),
            pltpu.VMEM((1, width), f32),
            pltpu.VMEM((n_ep, top_count, rows), jnp.int32),
            pltpu.VMEM((n_ep, top_count, rows), f32),
            pltpu.VMEM((width, hidden), bf16),
            pltpu.VMEM((width, hidden), bf16),
            pltpu.VMEM((hidden, width), bf16),
            pltpu.VMEM((shared, width), bf16),
            pltpu.VMEM((shared, width), bf16),
            pltpu.VMEM((shared, width), bf16),
            pltpu.VMEM((n_ep - 1, rows, width), bf16),
            pltpu.VMEM((n_ep, CORES, chips, rows, out_cols), bf16),
            pltpu.VMEM((n_ep, chips, rows, out_cols), bf16),
            pltpu.VMEM((n_ep, chips, rows, out_cols), bf16),
            pltpu.VMEM((n_ep, chips - 1, rows, out_cols), bf16),
            pltpu.VMEM((n_ep - 1, rows, out_cols), bf16),
            pltpu.VMEM((n_ep - 1, rows, out_cols), bf16),
            pltpu.VMEM((rows, out_cols), f32),
            dma((len(operands),)),
            dma((3, n_ep - 1)),
            dma((3, n_ep - 1)),
            dma((groups, chips - 1)),
            dma((groups, chips - 1)),
            dma((groups, chips)),
            dma((groups, chips)),
            dma((groups + 1, chips)),
            dma((groups + 1, chips)),
            dma((groups + 1, chips - 1)),
            dma((groups + 1, chips - 1)),
            dma((n_ep - 1,)),
            dma((n_ep - 1,)),
        ],
        compiler_params=pltpu.CompilerParams(
            collective_id=0, has_side_effects=True, vmem_limit_bytes=60 * 1024 * 1024
        ),
    )(*operands)


def solution(mesh):
    in_specs = (
        P(("grp", "ep"), None),
        P(),
        P(("grp", "ep"), None),
        P(("grp", "ep"), None),
        P(("ep", "tp"), None, None),
        P(("ep", "tp"), None, None),
        P(("ep", "tp"), None, None),
        P(None, "tp"),
        P(None, "tp"),
        P("tp", None),
    )
    out_specs = P(("grp", "ep"), "tp")
    return jax.shard_map(
        per_device, mesh=mesh, in_specs=in_specs, out_specs=out_specs, check_vma=False
    )
```

```python
import functools

import jax
import jax.numpy as jnp
from jax import lax
from jax.experimental import pallas as pl
from jax.experimental.pallas import tpu as pltpu
from jax.sharding import PartitionSpec as P

EXPERT_SHARDS = 2
CORES = 2
MESH = pl.DeviceIdType.MESH

eps = 1e-06
routed_scale = 2.5


def norm_rows(tokens, norm_gain):
    values = tokens.astype(jnp.float32)
    scaled = values * lax.rsqrt(jnp.mean(values * values, axis=-1, keepdims=True) + eps)
    return (scaled * norm_gain).astype(jnp.bfloat16)


def silu(value):
    return value / (1.0 + jnp.exp(-value))


def kernel(
    n_ep,
    n_tp,
    tok_hbm,
    gain_hbm,
    routes_hbm,
    score_hbm,
    gate_hbm,
    up_hbm,
    down_hbm,
    sgate_hbm,
    sup_hbm,
    sdown_hbm,
    out_ref,
    tok,
    gain,
    routes,
    score,
    gate,
    up,
    down,
    sgate,
    sup,
    sdown,
    gathered,
    part,
    part_in,
    pair,
    pair_in,
    plane,
    plane_in,
    kept,
    load_sem,
    z_send,
    z_recv,
    xy_send,
    xy_recv,
    d2d_send,
    d2d_recv,
    a_send,
    a_recv,
    b_send,
    b_recv,
    c_send,
    c_recv,
):
    chips = n_tp // CORES
    me = lax.axis_index("ep")
    seat = lax.axis_index("tp")
    chip, core = seat // CORES, seat % CORES
    rows, width = tok.shape
    half = rows // CORES
    chip_cols = width // chips
    out_cols = width // n_tp
    groups = group_count(n_ep)
    span = (n_ep - 1) // groups
    expert = me * (n_tp // EXPERT_SHARDS) + chip

    partner = {"tp": chip * CORES + 1 - core}
    plane_chip = [flipped(chip, j, chips) for j in range(chips)]
    plane_order = list(range(chips - 1, 0, -1))
    plane_peer = [{"tp": c * CORES + core} for c in plane_chip]
    others = [me] + [source_of(me, d, n_ep) for d in range(n_ep - 1, 0, -1)]
    forward = [{"ep": other} for other in others]

    def remote(src, dst, send, recv, target):
        return pltpu.make_async_remote_copy(
            src_ref=src, dst_ref=dst, send_sem=send, recv_sem=recv, device_id=target, device_id_type=MESH
        )

    loads = [
        pltpu.make_async_copy(src, dst, load_sem.at[i])
        for i, (src, dst) in enumerate(
            [
                (tok_hbm, tok),
                (routes_hbm, routes.at[0]),
                (score_hbm, score.at[0]),
                (gain_hbm, gain),
                (gate_hbm.at[0], gate),
                (up_hbm.at[0], up),
                (sgate_hbm, sgate),
                (sup_hbm, sup),
                (down_hbm.at[0], down),
                (sdown_hbm, sdown),
            ]
        )
    ]
    for load in loads:
        load.start()

    barrier = pltpu.get_barrier_semaphore()
    targets = forward[1:] + plane_peer[1:] + [partner]
    for target in targets:
        pl.semaphore_signal(barrier, inc=1, device_id=target, device_id_type=MESH)
    for load in loads[:3]:
        load.wait()
    pl.semaphore_wait(barrier, len(targets))

    my_rows = pl.ds(pl.multiple_of(core * half, half), half)
    my_cols = pl.ds(pl.multiple_of(chip * chip_cols, chip_cols), chip_cols)

    def z_pieces(source, slot, target):
        return [
            remote(
                tok.at[my_rows, my_cols],
                gathered.at[slot - 1, my_rows, my_cols],
                z_send.at[0, source],
                z_recv.at[0, slot - 1],
                target,
            ),
            remote(routes.at[0], routes.at[slot], z_send.at[1, source], z_recv.at[1, slot - 1], target),
            remote(score.at[0], score.at[slot], z_send.at[2, source], z_recv.at[2, slot - 1], target),
        ]

    z_copies = [z_pieces(d - 1, place_of(me, others[d], n_ep), forward[d]) for d in range(1, n_ep)]
    z_arrivals = [z_pieces(slot - 1, slot, forward[1]) for slot in range(1, n_ep)]
    for piece in range(3):
        for copies in z_copies:
            copies[piece].start()

    diagonal = lax.broadcasted_iota(jnp.int32, (rows, rows), 0) == lax.broadcasted_iota(
        jnp.int32, (rows, rows), 1
    )

    def row_weight(slot):
        scores = score[slot]
        mixing = scores / jnp.sum(scores, axis=0, keepdims=True) * routed_scale
        lane = jnp.sum(jnp.where(routes[slot] == expert, mixing, 0.0), axis=0, keepdims=True)
        return jnp.sum(jnp.where(diagonal, lane, 0.0), axis=1, keepdims=True)

    def span_of(group):
        if group == 0:
            return 0, 1
        return 1 + (group - 1) * span, span

    a_copies, b_copies = [], []

    def compute(group):
        first, count = span_of(group)
        raw = tok[...] if group == 0 else gathered[first - 1 : first - 1 + count].reshape(count * rows, width)
        normed = norm_rows(raw, gain[...])
        if group == 0:
            for load in loads[4:8]:
                load.wait()
        gate_part = jnp.dot(normed, gate[...], preferred_element_type=jnp.float32)
        upper = jnp.dot(normed, up[...], preferred_element_type=jnp.float32)
        weight = [row_weight(slot) for slot in range(first, first + count)]
        weight = weight[0] if count == 1 else jnp.concatenate(weight, axis=0)
        active = (silu(gate_part) * upper * weight).astype(jnp.bfloat16)
        if group == 0:
            contract = (((1,), (1,)), ((), ()))
            shared_gate = lax.dot_general(normed, sgate[...], contract, preferred_element_type=jnp.float32)
            shared_up = lax.dot_general(normed, sup[...], contract, preferred_element_type=jnp.float32)
            shared = (silu(shared_gate) * shared_up).astype(jnp.bfloat16)
            for load in loads[8:]:
                load.wait()
        copies = [None] * chips
        for j in plane_order + [0]:
            c = plane_chip[j]
            cols = pl.ds(pl.multiple_of(c * chip_cols, chip_cols), chip_cols)
            value = jnp.dot(active, down[:, cols], preferred_element_type=jnp.float32)
            if group == 0:
                value = value + jnp.dot(shared, sdown[:, cols], preferred_element_type=jnp.float32)
            value = value.astype(jnp.bfloat16)
            for s in range(count):
                for k in range(CORES):
                    part[first + s, k, c] = value[
                        s * rows : (s + 1) * rows, k * out_cols : (k + 1) * out_cols
                    ]
            copies[j] = remote(
                part.at[pl.ds(first, count), 1 - core, c],
                part_in.at[pl.ds(first, count), c],
                a_send.at[group, j],
                a_recv.at[group, j],
                partner,
            )
            copies[j].start()
        a_copies.append(copies)

    def pair_sum(slots, c):
        return part[slots, core, c].astype(jnp.float32) + part_in[slots, c].astype(jnp.float32)

    def reduce_pair(group):
        first, count = span_of(group)
        slots = pl.ds(first, count)
        copies = [None] * chips
        for j in plane_order:
            c = plane_chip[j]
            a_copies[group][j].wait_recv()
            pair[slots, c] = pair_sum(slots, c).astype(jnp.bfloat16)
            copies[j] = remote(
                pair.at[slots, c],
                pair_in.at[slots, j - 1],
                b_send.at[group, j - 1],
                b_recv.at[group, j - 1],
                plane_peer[j],
            )
            copies[j].start()
        a_copies[group][0].wait_recv()
        b_copies.append(copies)

    c_copies = []

    def reduce_plane(group):
        first, count = span_of(group)
        slots = pl.ds(first, count)
        total = pair_sum(slots, chip)
        for j in range(1, chips):
            b_copies[group][j].wait_recv()
            total = total + pair_in[slots, j - 1].astype(jnp.float32)
        if group == 0:
            kept[...] = total[0]
            return
        plane[pl.ds(first - 1, count)] = total.astype(jnp.bfloat16)
        for d in range(first, first + count):
            source = source_of(me, d, n_ep)
            there = lax.rem(source - me + n_ep, n_ep) - 1
            copy = remote(
                plane.at[d - 1], plane_in.at[there], c_send.at[d - 1], c_recv.at[there], {"ep": source}
            )
            copy.start()
            c_copies.append(copy)

    xy_copies, d2d_copies = [], []

    def block_of(group, c):
        first, count = span_of(group)
        cols = pl.ds(pl.multiple_of(c * chip_cols, chip_cols), chip_cols)
        return gathered.at[pl.ds(first - 1, count), my_rows, cols]

    def swap_piece(group, j):
        block = block_of(group, plane_chip[j])
        copy = remote(block, block, d2d_send.at[group - 1, j], d2d_recv.at[group - 1, j], partner)
        copy.start()
        d2d_copies[group - 1].append(copy)

    def spread(group):
        first, count = span_of(group)
        for d in range(first, first + count):
            z_arrivals[d - 1][0].wait_recv()
        block = block_of(group, chip)
        copies = [None] * chips
        for j in plane_order:
            copies[j] = remote(
                block, block, xy_send.at[group - 1, j - 1], xy_recv.at[group - 1, j - 1], plane_peer[j]
            )
            copies[j].start()
        xy_copies.append(copies)
        d2d_copies.append([])
        swap_piece(group, 0)

    def swap(group):
        for j in plane_order[::-1]:
            xy_copies[group - 1][j].wait_recv()
            swap_piece(group, j)

    def arrive(group):
        first, count = span_of(group)
        for d in range(first, first + count):
            z_arrivals[d - 1][1].wait_recv()
            z_arrivals[d - 1][2].wait_recv()
        for copy in d2d_copies[group - 1]:
            copy.wait_recv()

    loads[3].wait()
    compute(0)
    for group in range(1, groups + 1):
        spread(group)
    reduce_pair(0)
    swap(1)
    for group in range(1, groups + 1):
        if group < groups:
            swap(group + 1)
        if group > 1:
            reduce_pair(group - 1)
        arrive(group)
        compute(group)
    reduce_pair(groups)
    for group in range(groups + 1):
        reduce_plane(group)
    total = kept[...]
    for d in range(1, n_ep):
        remote(
            plane.at[0], plane_in.at[d - 1], c_send.at[d - 1], c_recv.at[d - 1], forward[1]
        ).wait_recv()
        total = total + plane_in[d - 1].astype(jnp.float32)
    out_ref[...] = total.astype(jnp.bfloat16)
    everything = sum(z_copies + xy_copies + b_copies + d2d_copies + a_copies, []) + c_copies
    for copy in everything:
        if copy is not None:
            copy.wait_send()


def flipped(chip, j, chips):
    assert chips & (chips - 1) == 0
    out, bit = chip, 1
    while bit < chips:
        if j & bit:
            out = out + bit - 2 * bit * (chip // bit % 2)
        bit *= 2
    return out


def room(index, count):
    side = jnp.minimum(index, count - 1 - index)
    toward = jnp.where(index < count - 1 - index, 1, -1)
    return side, toward


def source_of(index, place, count):
    side, toward = room(index, count)
    near = (place + 1) // 2 * (1 if place % 2 else -1)
    return index + toward * jnp.where(place <= 2 * side, near, place - side)


def place_of(source, index, count):
    side, toward = room(index, count)
    away = jnp.abs(source - index)
    same = (source - index) * toward > 0
    return jnp.where(away <= side, 2 * away - jnp.where(same, 1, 0), away + side)


def group_count(n_ep):
    return 3 if (n_ep - 1) % 3 == 0 else n_ep - 1


def per_device(
    tokens,
    norm_gain,
    routes,
    route_weight,
    gate_proj,
    up_proj,
    down_proj,
    shared_gate,
    shared_up,
    shared_down,
):
    n_ep = lax.axis_size("ep")
    n_tp = lax.axis_size("tp")
    chips = n_tp // CORES
    rows, width = tokens.shape
    out_cols = width // n_tp
    top_count = routes.shape[1]
    hidden = gate_proj.shape[2]
    shared = shared_gate.shape[1]
    groups = group_count(n_ep)
    bf16, f32 = jnp.bfloat16, jnp.float32
    dma = pltpu.SemaphoreType.DMA
    operands = (
        tokens,
        norm_gain.reshape(1, width),
        routes.T,
        route_weight.T,
        gate_proj,
        up_proj,
        down_proj,
        shared_gate.T,
        shared_up.T,
        shared_down,
    )
    return pl.pallas_call(
        functools.partial(kernel, n_ep, n_tp),
        out_shape=pltpu.VMEM((rows, out_cols), bf16),
        in_specs=[pl.BlockSpec(memory_space=pl.ANY)] * len(operands),
        out_specs=pl.BlockSpec(memory_space=pltpu.VMEM),
        scratch_shapes=[
            pltpu.VMEM((rows, width), bf16),
            pltpu.VMEM((1, width), f32),
            pltpu.VMEM((n_ep, top_count, rows), jnp.int32),
            pltpu.VMEM((n_ep, top_count, rows), f32),
            pltpu.VMEM((width, hidden), bf16),
            pltpu.VMEM((width, hidden), bf16),
            pltpu.VMEM((hidden, width), bf16),
            pltpu.VMEM((shared, width), bf16),
            pltpu.VMEM((shared, width), bf16),
            pltpu.VMEM((shared, width), bf16),
            pltpu.VMEM((n_ep - 1, rows, width), bf16),
            pltpu.VMEM((n_ep, CORES, chips, rows, out_cols), bf16),
            pltpu.VMEM((n_ep, chips, rows, out_cols), bf16),
            pltpu.VMEM((n_ep, chips, rows, out_cols), bf16),
            pltpu.VMEM((n_ep, chips - 1, rows, out_cols), bf16),
            pltpu.VMEM((n_ep - 1, rows, out_cols), bf16),
            pltpu.VMEM((n_ep - 1, rows, out_cols), bf16),
            pltpu.VMEM((rows, out_cols), f32),
            dma((len(operands),)),
            dma((3, n_ep - 1)),
            dma((3, n_ep - 1)),
            dma((groups, chips - 1)),
            dma((groups, chips - 1)),
            dma((groups, chips)),
            dma((groups, chips)),
            dma((groups + 1, chips)),
            dma((groups + 1, chips)),
            dma((groups + 1, chips - 1)),
            dma((groups + 1, chips - 1)),
            dma((n_ep - 1,)),
            dma((n_ep - 1,)),
        ],
        compiler_params=pltpu.CompilerParams(
            collective_id=0, has_side_effects=True, vmem_limit_bytes=60 * 1024 * 1024
        ),
    )(*operands)


def solution(mesh):
    in_specs = (
        P(("grp", "ep"), None),
        P(),
        P(("grp", "ep"), None),
        P(("grp", "ep"), None),
        P(("ep", "tp"), None, None),
        P(("ep", "tp"), None, None),
        P(("ep", "tp"), None, None),
        P(None, "tp"),
        P(None, "tp"),
        P("tp", None),
    )
    out_specs = P(("grp", "ep"), "tp")
    return jax.shard_map(
        per_device, mesh=mesh, in_specs=in_specs, out_specs=out_specs, check_vma=False
    )
```
